32 devices in a mesh: fs: 4 (over y, x), tp: 8 (over z, core).
Axes of the slice: x: 2, y: 2, z: 4, core: 2. Of those that a mesh axis runs over, the one named last changes fastest.
Arguments:
- value_input: bfloat16 [8192, 2048], P('fs', 'tp'), may hold values from -50 to 50
- value_cotangent: bfloat16 [8192, 512], P('fs'), may hold values from -6 to 6
- value_factor: bfloat16 [512, 128], replicated, may hold values from -10 to 10
- value_master: float32 [512, 2048], P('fs', 'tp'), may hold values from -0.125 to 0.125
- value_first: float32 [128, 2048], P('fs', 'tp'), may hold values from -4 to 4
- value_second: float32 [128, 2048], P('fs', 'tp'), may hold values from 0.01 to 0.2
- mixed_heads: bfloat16 [8192, 1024], P('fs', 'tp'), may hold values from -6 to 6
- output_cotangent: bfloat16 [8192, 2048], P('fs', 'tp'), may hold values from -50 to 50
- output_factor: bfloat16 [1024, 128], replicated, may hold values from -10 to 10
- output_master: float32 [1024, 2048], P('fs', 'tp'), may hold values from -0.1875 to 0.1875
- output_first: float32 [128, 2048], P('fs', 'tp'), may hold values from -4 to 4
- output_second: float32 [128, 2048], P('fs', 'tp'), may hold values from 0.01 to 0.2
Outputs:
- value_step: float32 [512, 2048], P('fs', 'tp')
- value_new_master: float32 [512, 2048], P('fs', 'tp')
- value_copy: bfloat16 [512, 2048], P(None, 'tp')
- value_first_new: float32 [128, 2048], P('fs', 'tp')
- value_second_new: float32 [128, 2048], P('fs', 'tp')
- output_step: float32 [1024, 2048], P('fs', 'tp')
- output_new_master: float32 [1024, 2048], P('fs', 'tp')
- output_copy: bfloat16 [1024, 2048], P(None, 'tp')
- output_first_new: float32 [128, 2048], P('fs', 'tp')
- output_second_new: float32 [128, 2048], P('fs', 'tp')
The draws below stay inside these ranges and needn't reach their ends.
All inputs are finite; a program needn't handle non-finite values.
Results may differ from the reference program's by a relative error of at most 0.001.
Values may be sent and summed in bfloat16 or wider, within the bound.
No kernel may reach another device: no remote copies, remote signals or barrier semaphores. Data moves between devices by JAX's collectives and lax.ppermute only.
A program may use at most 64 MiB of HBM per device.

```python
import math
import jax
import jax.numpy as jnp
from jax import lax

D = 2048
RANK = 128
HW = 1024
VW = 512
TOKENS = 8192


def column_scaled(key, rows, cols):
    key_rough, key_own = jax.random.split(key, 2)
    ramp = 10.0 ** (jnp.arange(cols, dtype=jnp.float32) / (cols - 1))
    rough = jnp.exp(jax.random.uniform(key_rough, (cols,), jnp.float32, -0.35, 0.35))
    base = jnp.clip(jax.random.normal(key_own, (rows, cols), jnp.float32), -3.5, 3.5)
    return base * ramp[None, :] * rough[None, :]


def draw_value_input(key, part):
    return column_scaled(jax.random.fold_in(key, 11), TOKENS, D).astype(jnp.bfloat16)


def draw_output_cotangent(key, part):
    return column_scaled(jax.random.fold_in(key, 12), TOKENS, D).astype(jnp.bfloat16)


def draw_value_factor(key, part):
    return (column_scaled(jax.random.fold_in(key, 13), VW, RANK) * VW ** (-0.5)).astype(jnp.bfloat16)


def draw_output_factor(key, part):
    return (column_scaled(jax.random.fold_in(key, 14), HW, RANK) * HW ** (-0.5)).astype(jnp.bfloat16)


def level_of(rng, dims, shards, least, largest):
    gain = 1.0
    for position, parts in shards:
        draws = jax.random.uniform(jax.random.fold_in(jax.random.fold_in(rng, 6), position), (parts,), jnp.float32, least / len(shards), largest / len(shards))
        gain = gain * jnp.repeat(jnp.exp(draws), dims[position] // parts).reshape((-1,) + (1,) * (len(dims) - 1 - position))
    return gain


def scatter_about(own_key, dims, scale, bound, cuts=(), kind=jnp.bfloat16):
    result = jax.random.normal(own_key, dims, jnp.float32) * scale
    if len(cuts) > 0:
        result = level_of(own_key, dims, cuts, -0.22, 0.18) * result
    return jnp.clip(result, min=-bound, max=bound).astype(kind)


def setup_inputs(seed: int = 0) -> dict:
    splits = jax.random.split(jax.random.key(seed), 13)
    value_input = draw_value_input(jax.random.fold_in(splits[12], 71), 0)
    value_cotangent = scatter_about(splits[1], (TOKENS, VW), 1.0, 6.0, ((0, 4),))
    value_factor = draw_value_factor(jax.random.fold_in(splits[12], 71), 0)
    value_master = scatter_about(splits[3], (VW, D), D ** -0.5, 0.125, ((0, 4), (1, 8)), jnp.float32)
    value_first = scatter_about(splits[4], (RANK, D), 0.3, 4.0, ((0, 4), (1, 8)), jnp.float32)
    value_second = jnp.clip(jnp.exp(math.log(0.2) - 2.9957323 * jax.random.uniform(splits[5], (RANK, D), jnp.float32) ** level_of(splits[5], (RANK, D), ((0, 4), (1, 8)), -0.2, 0.2)), 0.01, 0.2)
    mixed_heads = scatter_about(splits[6], (TOKENS, HW), 1.0, 6.0, ((0, 4), (1, 8)))
    output_cotangent = draw_output_cotangent(jax.random.fold_in(splits[12], 71), 0)
    output_factor = draw_output_factor(jax.random.fold_in(splits[12], 71), 0)
    output_master = scatter_about(splits[9], (HW, D), HW ** -0.5, 0.1875, ((0, 4), (1, 8)), jnp.float32)
    output_first = scatter_about(splits[10], (RANK, D), 0.3, 4.0, ((0, 4), (1, 8)), jnp.float32)
    output_second = jnp.clip(jnp.exp(math.log(0.2) - 2.9957323 * jax.random.uniform(splits[11], (RANK, D), jnp.float32) ** level_of(splits[11], (RANK, D), ((0, 4), (1, 8)), -0.2, 0.2)), 0.01, 0.2)
    return {"value_input": value_input, "value_cotangent": value_cotangent, "value_factor": value_factor, "value_master": value_master, "value_first": value_first, "value_second": value_second, "mixed_heads": mixed_heads, "output_cotangent": output_cotangent, "output_factor": output_factor, "output_master": output_master, "output_first": output_first, "output_second": output_second}


highest = lax.Precision.HIGHEST

def adam_part(projected, first, second, factor, master):
    scale = lax.rsqrt(jnp.mean(projected * projected) + 1e-06)
    scaled = scale * projected
    first_new = 0.9 * first + 0.1 * scaled
    second_new = 0.95 * second + 0.05 * scaled * scaled
    direction = first_new / (jnp.sqrt(second_new) + 1e-08)
    step = jnp.dot(factor.astype(jnp.float32), direction, precision=highest, preferred_element_type=jnp.float32)
    new_master = master - 0.002 * step
    return (step, new_master, new_master.astype(jnp.bfloat16), first_new, second_new)

def reference(value_input, value_cotangent, value_factor, value_master, value_first, value_second, mixed_heads, output_cotangent, output_factor, output_master, output_first, output_second):
    value_image = jnp.dot(value_cotangent.astype(jnp.float32), value_factor.astype(jnp.float32), precision=highest, preferred_element_type=jnp.float32)
    value_projected = jnp.dot(value_image.T, value_input.astype(jnp.float32), precision=highest, preferred_element_type=jnp.float32)
    output_image = jnp.dot(mixed_heads.astype(jnp.float32), output_factor.astype(jnp.float32), precision=highest, preferred_element_type=jnp.float32)
    output_projected = jnp.dot(output_image.T, output_cotangent.astype(jnp.float32), precision=highest, preferred_element_type=jnp.float32)
    value_out = adam_part(value_projected, value_first, value_second, value_factor, value_master)
    output_out = adam_part(output_projected, output_first, output_second, output_factor, output_master)
    return (value_out[0], value_out[1], value_out[2], value_out[3], value_out[4], output_out[0], output_out[1], output_out[2], output_out[3], output_out[4])
```

```python
import functools

import jax
import jax.numpy as jnp
from jax import lax
from jax.experimental import pallas as pl
from jax.experimental.pallas import tpu as pltpu
from jax.sharding import PartitionSpec as P


highest = lax.Precision.HIGHEST
f32 = jnp.float32
bf16 = jnp.bfloat16


def send_xor(x, axis, step):
    count = lax.axis_size(axis)
    return lax.ppermute(x, axis, [(i, i ^ step) for i in range(count)])


def dot_split(left, right):
    high = right.astype(bf16)
    low = (right - high.astype(f32)).astype(bf16)
    return jnp.dot(left, high, preferred_element_type=f32) + jnp.dot(
        left, low, preferred_element_type=f32
    )


def finish_side(me, scale, projected, packs, offset, rows, factor, outs, direction, band):
    step_out, new_out, copy_out, first_out, second_out = outs
    for k, pack in enumerate(packs):
        at = pl.multiple_of((me ^ k) * band, band)
        scaled = scale * projected[pl.ds(at, band), :]
        first = 0.9 * pack[offset : offset + band, :] + 0.1 * scaled
        second = 0.95 * pack[offset + band : offset + 2 * band, :] + 0.05 * scaled * scaled
        if k == 0:
            first_out[...] = first
            second_out[...] = second
        direction[pl.ds(at, band), :] = first / (jnp.sqrt(second) + 1e-08)
    high = direction[...].astype(bf16)
    low = (direction[...] - high.astype(f32)).astype(bf16)
    for k, pack in enumerate(packs):
        at = pl.multiple_of((me ^ k) * rows, rows)
        own = factor[pl.ds(at, rows), :]
        step = jnp.dot(own, high, preferred_element_type=f32) + jnp.dot(
            own, low, preferred_element_type=f32
        )
        base = offset_master(offset, band, rows)
        new = pack[base : base + rows, :] - 0.002 * step
        copy_out[pl.ds(at, rows), :] = new.astype(bf16)
        if k == 0:
            step_out[...] = step
            new_out[...] = new


def offset_master(offset, band, rows):
    return offset + 2 * band


def finish_kernel(count, band, value_rows, output_rows, *refs):
    me_ref, scale_ref, value_proj, output_proj, value_factor, output_factor = refs[:6]
    packs = refs[6 : 6 + count]
    value_outs = refs[6 + count : 11 + count]
    output_outs = refs[11 + count : 16 + count]
    direction = refs[16 + count]
    me = me_ref[0]
    finish_side(
        me, scale_ref[0], value_proj, packs, 0, value_rows, value_factor, value_outs, direction, band
    )
    finish_side(
        me,
        scale_ref[1],
        output_proj,
        packs,
        2 * band + value_rows,
        output_rows,
        output_factor,
        output_outs,
        direction,
        band,
    )


def finish(me, scales, value_proj, output_proj, value_factor, output_factor, packs, value_rows, output_rows):
    count = len(packs)
    rank, columns = value_proj.shape
    band = rank // count
    smem = pl.BlockSpec(memory_space=pltpu.SMEM)
    vmem = pl.BlockSpec(memory_space=pltpu.VMEM)

    def side(rows):
        return [
            jax.ShapeDtypeStruct((rows, columns), f32),
            jax.ShapeDtypeStruct((rows, columns), f32),
            jax.ShapeDtypeStruct((rows * count, columns), bf16),
            jax.ShapeDtypeStruct((band, columns), f32),
            jax.ShapeDtypeStruct((band, columns), f32),
        ]

    outs = side(value_rows) + side(output_rows)
    return pl.pallas_call(
        functools.partial(finish_kernel, count, band, value_rows, output_rows),
        out_shape=outs,
        in_specs=[smem, smem] + [vmem] * (4 + count),
        out_specs=[vmem] * 10,
        scratch_shapes=[pltpu.VMEM((rank, columns), f32)],
        name="finish",
    )(me, scales, value_proj, output_proj, value_factor, output_factor, *packs)


def on_device(
    value_input,
    value_cotangent,
    value_factor,
    value_master,
    value_first,
    value_second,
    mixed_heads,
    output_cotangent,
    output_factor,
    output_master,
    output_first,
    output_second,
):
    fs_count = lax.axis_size("fs")
    fs_place = lax.axis_index("fs")
    tp_count = lax.axis_size("tp")
    tp_place = lax.axis_index("tp")
    chips = tp_count // 2
    core = tp_place % 2
    chip = tp_place // 2
    rank = value_factor.shape[1]
    columns = value_input.shape[1]
    tokens, features = mixed_heads.shape
    half = tokens // 2
    chunk = half // chips

    def rows_of(x, start, size):
        return lax.dynamic_slice_in_dim(x, start, size, 0)

    heads_other = send_xor(rows_of(mixed_heads, (1 - core) * half, half), "tp", 1)
    heads_own = rows_of(mixed_heads, core * half, half)

    pack = jnp.concatenate(
        [value_first, value_second, value_master, output_first, output_second, output_master], axis=0
    )
    packs = [pack] + [send_xor(pack, "fs", k) for k in range(1, fs_count)]

    value_image = jnp.dot(value_cotangent, value_factor, preferred_element_type=f32)

    def project(image, cotangent):
        return lax.dot_general(
            image,
            cotangent.astype(f32),
            (((0,), (0,)), ((), ())),
            precision=highest,
            preferred_element_type=f32,
        )

    def over_fs(term):
        terms = [term] + [send_xor(term, "fs", k) for k in range(1, fs_count)]
        while len(terms) > 1:
            terms = [terms[2 * i] + terms[2 * i + 1] for i in range(len(terms) // 2)]
        return terms[0]

    value_proj = over_fs(project(value_image, value_input))

    factor_own = rows_of(output_factor, tp_place * features, features)
    factor_other = rows_of(output_factor, (tp_place ^ 1) * features, features)
    partial = jnp.dot(heads_own, factor_own, preferred_element_type=f32) + jnp.dot(
        heads_other, factor_other, preferred_element_type=f32
    )
    total = rows_of(partial, chip * chunk, chunk)
    for k in range(1, chips):
        total = total + send_xor(rows_of(partial, (chip ^ k) * chunk, chunk), "tp", 2 * k)
    image_half = jnp.zeros((half, rank), f32)
    image_half = lax.dynamic_update_slice_in_dim(image_half, total, chip * chunk, 0)
    for k in range(1, chips):
        image_half = lax.dynamic_update_slice_in_dim(
            image_half, send_xor(total, "tp", 2 * k), (chip ^ k) * chunk, 0
        )
    image_other = send_xor(image_half, "tp", 1)
    output_term = project(image_half, rows_of(output_cotangent, core * half, half)) + project(
        image_other, rows_of(output_cotangent, (1 - core) * half, half)
    )
    output_proj = over_fs(output_term)

    squares = jnp.stack([jnp.sum(value_proj * value_proj), jnp.sum(output_proj * output_proj)])
    squares = jnp.broadcast_to(squares[:, None], (2, 128))
    pair = squares + send_xor(squares, "tp", 1)
    whole = [pair] + [send_xor(pair, "tp", 2 * k) for k in range(1, chips)]
    while len(whole) > 1:
        whole = [whole[2 * i] + whole[2 * i + 1] for i in range(len(whole) // 2)]
    scales = lax.rsqrt(whole[0][:, 0] / (rank * columns * tp_count) + 1e-06)
    return tuple(
        finish(
            fs_place.reshape(1).astype(jnp.int32),
            scales,
            value_proj,
            output_proj,
            value_factor,
            output_factor,
            packs,
            value_master.shape[0],
            output_master.shape[0],
        )
    )


def solution(mesh):
    in_specs = (
        P("fs", "tp"),
        P("fs", None),
        P(),
        P("fs", "tp"),
        P("fs", "tp"),
        P("fs", "tp"),
        P("fs", "tp"),
        P("fs", "tp"),
        P(),
        P("fs", "tp"),
        P("fs", "tp"),
        P("fs", "tp"),
    )
    out_specs = (
        P("fs", "tp"),
        P("fs", "tp"),
        P(None, "tp"),
        P("fs", "tp"),
        P("fs", "tp"),
        P("fs", "tp"),
        P("fs", "tp"),
        P(None, "tp"),
        P("fs", "tp"),
        P("fs", "tp"),
    )
    return jax.shard_map(
        on_device, mesh=mesh, in_specs=in_specs, out_specs=out_specs, check_vma=False
    )
```

```python
import functools

import jax
import jax.numpy as jnp
from jax import lax
from jax.experimental import pallas as pl
from jax.experimental.pallas import tpu as pltpu
from jax.sharding import PartitionSpec as P


SMALL = pltpu.CompilerParams(vmem_limit_bytes=16 * 2**20)
highest = lax.Precision.HIGHEST
f32 = jnp.float32
bf16 = jnp.bfloat16
f16 = jnp.float16


def send_xor(x, axis, step):
    count = lax.axis_size(axis)
    return lax.ppermute(x, axis, [(i, i ^ step) for i in range(count)])


def finish_side(me, scale, projected, blocks, rows, factor, outs, direction, band):
    step_out, new_out, copy_out, first_out, second_out = outs
    for k, (first_old, second_old, _) in enumerate(blocks):
        at = pl.multiple_of((me ^ k) * band, band)
        scaled = scale * projected[pl.ds(at, band), :]
        first = 0.9 * first_old[...] + 0.1 * scaled
        second = 0.95 * second_old[...] + 0.05 * scaled * scaled
        if k == 0:
            first_out[...] = first
            second_out[...] = second
        direction[pl.ds(at, band), :] = first / (jnp.sqrt(second) + 1e-08)
    high = direction[...].astype(bf16)
    low = (direction[...] - high.astype(f32)).astype(bf16)
    for k, (_, _, master) in enumerate(blocks):
        at = pl.multiple_of((me ^ k) * rows, rows)
        own = factor[pl.ds(at, rows), :]
        step = jnp.dot(own, high, preferred_element_type=f32) + jnp.dot(
            own, low, preferred_element_type=f32
        )
        new = master[...] - 0.002 * step
        copy_out[pl.ds(at, rows), :] = new.astype(bf16)
        if k == 0:
            step_out[...] = step
            new_out[...] = new


def finish_kernel(chips, places, entries, value_rows, output_rows, *refs):
    tiles, refs = refs[:chips], refs[chips:]
    value_proj, output_proj, value_factor, output_factor = refs[:4]
    outs, direction = refs[-11:-1], refs[-1]
    packs = refs[4:-11]
    me = lax.axis_index("fs")
    sums = [t[0:1, :] for t in tiles]
    while len(sums) > 1:
        sums = [sums[2 * i] + sums[2 * i + 1] for i in range(len(sums) // 2)]
    scales = lax.rsqrt(sums[0] / entries + 1e-06)
    band = direction.shape[0] // len(places)
    value_blocks, output_blocks = [], []
    for (small, at), (large, at_large) in places:
        cuts = [packs[small].at[at + i * band : at + (i + 1) * band, :] for i in range(4)]
        value_master = packs[small].at[at + 4 * band : at + 4 * band + value_rows, :]
        output_master = packs[large].at[at_large : at_large + output_rows, :]
        value_blocks.append((cuts[0], cuts[1], value_master))
        output_blocks.append((cuts[2], cuts[3], output_master))
    for scale, projected, blocks, rows, factor, side_outs in (
        (scales[:, 0:1], value_proj, value_blocks, value_rows, value_factor, outs[:5]),
        (scales[:, 64:65], output_proj, output_blocks, output_rows, output_factor, outs[5:]),
    ):
        finish_side(me, scale, projected, blocks, rows, factor, side_outs, direction, band)


def finish(tiles, entries, value_proj, output_proj, value_factor, output_factor, smalls, larges):
    count = len(smalls)
    rank, columns = value_proj.shape
    band = rank // count
    value_rows, output_rows = value_factor.shape[0] // count, output_factor.shape[0] // count
    vmem = pl.BlockSpec(memory_space=pltpu.VMEM)
    arrays = []

    def place(part):
        array, at = part
        for i, known in enumerate(arrays):
            if known is array:
                return i, at
        arrays.append(array)
        return len(arrays) - 1, at

    places = tuple((place(small), place(large)) for small, large in zip(smalls, larges))

    def side(rows):
        return [
            jax.ShapeDtypeStruct((rows, columns), f32),
            jax.ShapeDtypeStruct((rows, columns), f32),
            jax.ShapeDtypeStruct((rows * count, columns), bf16),
            jax.ShapeDtypeStruct((band, columns), f32),
            jax.ShapeDtypeStruct((band, columns), f32),
        ]

    return pl.pallas_call(
        functools.partial(finish_kernel, len(tiles), places, entries, value_rows, output_rows),
        out_shape=side(value_rows) + side(output_rows),
        in_specs=[vmem] * (len(tiles) + 4 + len(arrays)),
        out_specs=[vmem] * 10,
        scratch_shapes=[pltpu.VMEM((rank, columns), f32)],
        compiler_params=SMALL,
        name="finish",
    )(*tiles, value_proj, output_proj, value_factor, output_factor, *arrays)


def term_kernel(x, out):
    rank, columns = x.shape
    root = jnp.maximum(jnp.sqrt(largest_of(x)) * 0.25, 2.0**-14)
    wide = root * (2.0**23 + 1.0)
    root = 2.0 * (wide - (wide - root))
    out[0:rank, :] = x[...] * (2048.0 / (root * root))
    out[rank : rank + 16, :] = jnp.broadcast_to(root, (16, columns))


def scaled_term(x):
    vmem = pl.BlockSpec(memory_space=pltpu.VMEM)
    rank, columns = x.shape
    return pl.pallas_call(
        term_kernel,
        out_shape=jax.ShapeDtypeStruct((rank + 16, columns), f32),
        in_specs=[vmem],
        out_specs=vmem,
        compiler_params=SMALL,
        cost_estimate=pl.CostEstimate(flops=100_000_000, bytes_accessed=0, transcendentals=0),
        name="scaled_term",
    )(x)


def square_kernel(value, output, squares):
    def square(x):
        return jnp.sum(jnp.sum(x * x, axis=0, keepdims=True), axis=1, keepdims=True)

    lane = lax.broadcasted_iota(jnp.int32, squares.shape, 1)
    squares[...] = jnp.where(lane < 64, square(value[...]), square(output[...]))


def sum_squares(value, output):
    vmem = pl.BlockSpec(memory_space=pltpu.VMEM)
    return pl.pallas_call(
        square_kernel,
        out_shape=jax.ShapeDtypeStruct((8, 128), f32),
        in_specs=[vmem] * 2,
        out_specs=vmem,
        compiler_params=SMALL,
        cost_estimate=pl.CostEstimate(flops=100_000_000, bytes_accessed=0, transcendentals=0),
        name="sum_squares",
    )(value, output)


def largest_of(x):
    return jnp.max(jnp.max(jnp.abs(x[...]).astype(f32), axis=0, keepdims=True), axis=1, keepdims=True)


def first_kernel(chips, heads, factor, parts, rows_out, factor_other):
    tokens, features = heads.shape
    half, rank = tokens // 2, factor.shape[1]
    chunk = half // chips
    place = lax.axis_index("tp")
    core, chip = place & 1, place >> 1
    own_factor = factor[pl.ds(pl.multiple_of(place * features, features), features), :]
    factor_other[...] = factor[pl.ds(pl.multiple_of((place ^ 1) * features, features), features), :]
    for k in range(chips):
        at = pl.multiple_of(core * half + (chip ^ k) * chunk, chunk)
        parts[k * chunk : (k + 1) * chunk, :] = jnp.dot(
            heads[pl.ds(at, chunk), :], own_factor, preferred_element_type=f32
        )
    largest = jnp.maximum(largest_of(heads), 2.0**-13)
    bound = jnp.maximum(largest_of(factor), 1e-30) * (2 * features / 32768.0)
    rows_out[0:8, :] = jnp.broadcast_to(largest, (8, rank))
    rows_out[8:16, :] = jnp.broadcast_to(bound, (8, rank))


def second_kernel(chips, heads, parts, rows, factor, *outs):
    tokens, _ = heads.shape
    half, rank = tokens // 2, factor.shape[1]
    chunk = half // chips
    place = lax.axis_index("tp")
    core, chip = place & 1, place >> 1
    largest = jnp.maximum(rows[0:1, :], largest_of(heads))
    bound = rows[8:9, :]
    scale = 1.0 / (bound * largest)
    other_factor = factor[...]
    for k in reversed(range(chips)):
        at = pl.multiple_of(core * half + (chip ^ k) * chunk, chunk)
        part = parts[k * chunk : (k + 1) * chunk, :] + jnp.dot(
            heads[pl.ds(at, chunk), :], other_factor, preferred_element_type=f32
        )
        if k == 0:
            outs[0][...] = part
        else:
            outs[k][0:chunk, :] = part * scale
            outs[k][chunk : chunk + 16, :] = jnp.broadcast_to(largest, (16, rank))
    outs[chips][0:8, :] = jnp.broadcast_to(largest, (8, rank))
    outs[chips][8:16, :] = jnp.broadcast_to(bound, (8, rank))


def partial_image(heads, heads_other, factor, chips):
    tokens, features = heads.shape
    rank = factor.shape[1]
    chunk = tokens // (2 * chips)
    vmem = pl.BlockSpec(memory_space=pltpu.VMEM)
    cost = pl.CostEstimate(flops=200_000_000, bytes_accessed=0, transcendentals=0)
    parts, rows, other_factor = pl.pallas_call(
        functools.partial(first_kernel, chips),
        out_shape=[
            jax.ShapeDtypeStruct((tokens // 2, rank), f32),
            jax.ShapeDtypeStruct((16, rank), f32),
            jax.ShapeDtypeStruct((features, rank), bf16),
        ],
        in_specs=[vmem] * 2,
        out_specs=[vmem] * 3,
        compiler_params=SMALL,
        cost_estimate=cost,
        name="partial_first",
    )(heads, factor)
    return pl.pallas_call(
        functools.partial(second_kernel, chips),
        out_shape=[jax.ShapeDtypeStruct((chunk, rank), f32)]
        + [jax.ShapeDtypeStruct((chunk + 16, rank), f32)] * (chips - 1)
        + [jax.ShapeDtypeStruct((16, rank), f32)],
        in_specs=[vmem] * 4,
        out_specs=[vmem] * (chips + 1),
        compiler_params=SMALL,
        cost_estimate=cost,
        name="partial_second",
    )(heads_other, parts, rows, other_factor)


def pack_kernel(*refs):
    *sources, packed = refs
    at = 0
    for x in sources:
        packed[at : at + x.shape[0], :] = x[...]
        at += x.shape[0]


def pack_rows(*arrays):
    rows = sum(x.shape[0] for x in arrays)
    vmem = pl.BlockSpec(memory_space=pltpu.VMEM)
    return pl.pallas_call(
        pack_kernel,
        out_shape=jax.ShapeDtypeStruct((rows, arrays[0].shape[1]), f32),
        in_specs=[vmem] * len(arrays),
        out_specs=vmem,
        compiler_params=SMALL,
        cost_estimate=pl.CostEstimate(flops=100_000_000, bytes_accessed=0, transcendentals=0),
        name="pack_rows",
    )(*arrays)


def add_kernel(a, b, out):
    out[...] = a[...] + b[...]


def add_tiles(a, b):
    vmem = pl.BlockSpec(memory_space=pltpu.VMEM)
    return pl.pallas_call(
        add_kernel,
        out_shape=jax.ShapeDtypeStruct(a.shape, f32),
        in_specs=[vmem] * 2,
        out_specs=vmem,
        compiler_params=SMALL,
        name="add_tiles",
    )(a, b)


def on_device(
    value_input,
    value_cotangent,
    value_factor,
    value_master,
    value_first,
    value_second,
    mixed_heads,
    output_cotangent,
    output_factor,
    output_master,
    output_first,
    output_second,
):
    fs_count = lax.axis_size("fs")
    tp_count = lax.axis_size("tp")
    tp_place = lax.axis_index("tp")
    chips = tp_count // 2
    core = tp_place & 1
    chip = tp_place >> 1
    rank = value_factor.shape[1]
    columns = value_input.shape[1]
    tokens, _ = mixed_heads.shape
    half = tokens // 2
    chunk = half // chips

    def project(image, cotangent):
        return lax.dot_general(
            image,
            cotangent.astype(f32),
            (((0,), (0,)), ((), ())),
            precision=highest,
            preferred_element_type=f32,
        )

    def sum_fs(term):
        own = scaled_term(term).astype(f16)
        terms = [own]
        for k in range(1, fs_count):
            terms.append(send_xor(own, "fs", k))
        sums = []
        for t in terms:
            root = t[rank : rank + 1].astype(f32)
            sums.append(t[:rank].astype(f32) * (root * root * 2.0**-11))
        while len(sums) > 1:
            sums = [sums[2 * i] + sums[2 * i + 1] for i in range(len(sums) // 2)]
        return sums[0]

    def gather_fs(packed, cut):
        if fs_count != 4:
            whole = [packed]
            for k in range(1, fs_count):
                whole.append(send_xor(packed, "fs", k))
            return [(w, 0) for w in whole], [(w, cut) for w in whole]
        near = send_xor(packed, "fs", 1)
        far = send_xor(packed, "fs", 2)
        first = send_xor(near[:cut], "fs", 2)
        last = send_xor(far[cut:], "fs", 1)
        parts = [packed, near, far]
        return [(p, 0) for p in parts] + [(first, 0)], [(p, cut) for p in parts] + [(last, 0)]

    heads_other = send_xor(mixed_heads, "tp", 1)

    value_image = jnp.dot(value_cotangent, value_factor, preferred_element_type=f32)
    value_term = project(value_image, value_input)

    total, *sends, scale_rows = partial_image(
        mixed_heads, heads_other, output_factor, chips
    )
    largest, bound = scale_rows[0:1], scale_rows[8:9]
    arrived = []
    for k in range(1, chips):
        arrived.append(send_xor(sends[k - 1].astype(f16), "tp", 2 * k))
    for a in arrived:
        of_peer = a[chunk : chunk + 1].astype(f32)
        largest = jnp.maximum(largest, of_peer)
        total += a[:chunk].astype(f32) * (bound * of_peer)
    bound_total = bound * (chips * largest)
    total = (total * (1.0 / bound_total)).astype(f16)

    products = []
    for k in range(chips):
        mine = send_xor(total, "tp", 2 * k) if k else total
        theirs = send_xor(mine, "tp", 1)
        for at, part in ((core * half, mine), ((1 - core) * half, theirs)):
            rows = lax.dynamic_slice_in_dim(output_cotangent, at + (chip ^ k) * chunk, chunk, 0)
            product = project(part.astype(f32), rows)
            products.append(product)
    output_term = sum(products[1:], products[0]) * bound_total[0, 0]

    value_proj = sum_fs(value_term)
    output_proj = sum_fs(output_term)

    small = (value_first, value_second, output_first, output_second, value_master)
    packed = pack_rows(*small, output_master)
    smalls, larges = gather_fs(packed, sum(x.shape[0] for x in small))

    squares = sum_squares(value_proj, output_proj)
    squares = add_tiles(squares, send_xor(squares, "tp", 1))
    tiles = [squares]
    for k in range(1, chips):
        tiles.append(send_xor(squares, "tp", 2 * k))
    return tuple(
        finish(
            tiles,
            1.0 * rank * columns * tp_count,
            value_proj,
            output_proj,
            value_factor,
            output_factor,
            smalls,
            larges,
        )
    )


def solution(mesh):
    in_specs = (
        P("fs", "tp"),
        P("fs", None),
        P(),
        P("fs", "tp"),
        P("fs", "tp"),
        P("fs", "tp"),
        P("fs", "tp"),
        P("fs", "tp"),
        P(),
        P("fs", "tp"),
        P("fs", "tp"),
        P("fs", "tp"),
    )
    out_specs = (
        P("fs", "tp"),
        P("fs", "tp"),
        P(None, "tp"),
        P("fs", "tp"),
        P("fs", "tp"),
        P("fs", "tp"),
        P("fs", "tp"),
        P(None, "tp"),
        P("fs", "tp"),
        P("fs", "tp"),
    )
    return jax.shard_map(
        on_device, mesh=mesh, in_specs=in_specs, out_specs=out_specs, check_vma=False
    )
```

```python
import functools

import jax
import jax.numpy as jnp
from jax import lax
from jax.experimental import pallas as pl
from jax.experimental.pallas import tpu as pltpu
from jax.sharding import PartitionSpec as P


SMALL = pltpu.CompilerParams(vmem_limit_bytes=16 * 2**20)
highest = lax.Precision.HIGH
f32 = jnp.float32
bf16 = jnp.bfloat16
f16 = jnp.float16


def send_xor(x, axis, step):
    count = lax.axis_size(axis)
    return lax.ppermute(x, axis, [(i, i ^ step) for i in range(count)])


def send_split(x):
    return lax.ppermute(x, "tp", [(i, i ^ (6 if i & 1 else 2)) for i in range(8)])


def finish_side(me, scale, projected, blocks, rows, factor, outs, direction, band):
    step_out, new_out, copy_out, first_out, second_out = outs
    for k, (first_old, second_old, _) in enumerate(blocks):
        at = pl.multiple_of((me ^ k) * band, band)
        scaled = scale * projected[pl.ds(at, band), :]
        first = 0.9 * first_old[...] + 0.1 * scaled
        second = 0.95 * second_old[...] + 0.05 * scaled * scaled
        if k == 0:
            first_out[...] = first
            second_out[...] = second
        direction[pl.ds(at, band), :] = first / (jnp.sqrt(second) + 1e-08)
    high = direction[...].astype(bf16)
    low = (direction[...] - high.astype(f32)).astype(bf16)
    for k, (_, _, master) in enumerate(blocks):
        at = pl.multiple_of((me ^ k) * rows, rows)
        own = factor[pl.ds(at, rows), :]
        step = jnp.dot(own, high, preferred_element_type=f32) + jnp.dot(
            own, low, preferred_element_type=f32
        )
        new = master[...] - 0.002 * step
        copy_out[pl.ds(at, rows), :] = new.astype(bf16)
        if k == 0:
            step_out[...] = step
            new_out[...] = new


def finish_kernel(chips, places, entries, value_rows, output_rows, *refs):
    tiles, refs = refs[:chips], refs[chips:]
    value_proj, output_proj, value_factor, output_factor = refs[:4]
    outs, direction = refs[-11:-1], refs[-1]
    packs = refs[4:-11]
    me = lax.axis_index("fs")
    sums = [t[0:1, :] for t in tiles]
    while len(sums) > 1:
        sums = [sums[2 * i] + sums[2 * i + 1] for i in range(len(sums) // 2)]
    scales = lax.rsqrt(sums[0] / entries + 1e-06)
    band = direction.shape[0] // len(places)
    value_blocks, output_blocks = [], []
    for (small, at), (large, at_large) in places:
        cuts = [packs[small].at[at + i * band : at + (i + 1) * band, :] for i in range(4)]
        value_master = packs[small].at[at + 4 * band : at + 4 * band + value_rows, :]
        output_master = packs[large].at[at_large : at_large + output_rows, :]
        value_blocks.append((cuts[0], cuts[1], value_master))
        output_blocks.append((cuts[2], cuts[3], output_master))
    for scale, projected, blocks, rows, factor, side_outs in (
        (scales[:, 0:1], value_proj, value_blocks, value_rows, value_factor, outs[:5]),
        (scales[:, 64:65], output_proj, output_blocks, output_rows, output_factor, outs[5:]),
    ):
        finish_side(me, scale, projected, blocks, rows, factor, side_outs, direction, band)


def finish(tiles, entries, value_proj, output_proj, value_factor, output_factor, smalls, larges):
    count = len(smalls)
    rank, columns = value_proj.shape
    band = rank // count
    value_rows, output_rows = value_factor.shape[0] // count, output_factor.shape[0] // count
    vmem = pl.BlockSpec(memory_space=pltpu.VMEM)
    arrays = []

    def place(part):
        array, at = part
        for i, known in enumerate(arrays):
            if known is array:
                return i, at
        arrays.append(array)
        return len(arrays) - 1, at

    places = tuple((place(small), place(large)) for small, large in zip(smalls, larges))

    def side(rows):
        return [
            jax.ShapeDtypeStruct((rows, columns), f32),
            jax.ShapeDtypeStruct((rows, columns), f32),
            jax.ShapeDtypeStruct((rows * count, columns), bf16),
            jax.ShapeDtypeStruct((band, columns), f32),
            jax.ShapeDtypeStruct((band, columns), f32),
        ]

    return pl.pallas_call(
        functools.partial(finish_kernel, len(tiles), places, entries, value_rows, output_rows),
        out_shape=side(value_rows) + side(output_rows),
        in_specs=[vmem] * (len(tiles) + 4 + len(arrays)),
        out_specs=[vmem] * 10,
        scratch_shapes=[pltpu.VMEM((rank, columns), f32)],
        compiler_params=SMALL,
        name="finish",
    )(*tiles, value_proj, output_proj, value_factor, output_factor, *arrays)


def term_kernel(x, out):
    rank, columns = x.shape
    root = jnp.maximum(jnp.sqrt(largest_of(x)) * 0.25, 2.0**-14)
    wide = root * (2.0**23 + 1.0)
    root = 2.0 * (wide - (wide - root))
    out[0:rank, :] = x[...] * (2048.0 / (root * root))
    out[rank : rank + 16, :] = jnp.broadcast_to(root, (16, columns))


def scaled_term(x):
    vmem = pl.BlockSpec(memory_space=pltpu.VMEM)
    rank, columns = x.shape
    return pl.pallas_call(
        term_kernel,
        out_shape=jax.ShapeDtypeStruct((rank + 16, columns), f32),
        in_specs=[vmem],
        out_specs=vmem,
        compiler_params=SMALL,
        cost_estimate=pl.CostEstimate(flops=100_000_000, bytes_accessed=0, transcendentals=0),
        name="scaled_term",
    )(x)


def square_kernel(value, output, squares):
    def square(x):
        return jnp.sum(jnp.sum(x * x, axis=0, keepdims=True), axis=1, keepdims=True)

    lane = lax.broadcasted_iota(jnp.int32, squares.shape, 1)
    squares[...] = jnp.where(lane < 64, square(value[...]), square(output[...]))


def sum_squares(value, output):
    vmem = pl.BlockSpec(memory_space=pltpu.VMEM)
    return pl.pallas_call(
        square_kernel,
        out_shape=jax.ShapeDtypeStruct((8, 128), f32),
        in_specs=[vmem] * 2,
        out_specs=vmem,
        compiler_params=SMALL,
        cost_estimate=pl.CostEstimate(flops=100_000_000, bytes_accessed=0, transcendentals=0),
        name="sum_squares",
    )(value, output)


def largest_of(x):
    return jnp.max(jnp.max(jnp.abs(x[...]).astype(f32), axis=0, keepdims=True), axis=1, keepdims=True)


def first_kernel(chips, heads, factor, parts, rows_out):
    tokens, features = heads.shape
    half, rank = tokens // 2, factor.shape[1]
    chunk = half // chips
    place = lax.axis_index("tp")
    core, chip = place & 1, place >> 1
    own_factor = factor[pl.ds(pl.multiple_of(core * features, features), features), :]
    for k in range(chips):
        at = pl.multiple_of(core * half + (chip ^ k) * chunk, chunk)
        parts[k * chunk : (k + 1) * chunk, :] = jnp.dot(
            heads[pl.ds(at, chunk), :], own_factor, preferred_element_type=f32
        )
    rows_out[0:8, :] = jnp.broadcast_to(jnp.maximum(largest_of(heads), 2.0**-13), (8, rank))
    rows_out[8:16, :] = jnp.broadcast_to(jnp.maximum(largest_of(factor), 2.0**-13), (8, rank))


def second_kernel(chips, heads, parts, rows, factor, *outs):
    tokens, features = heads.shape
    half, rank = tokens // 2, factor.shape[1]
    chunk = half // chips
    place = lax.axis_index("tp")
    core, chip = place & 1, place >> 1
    largest = jnp.maximum(rows[0:1, :], largest_of(heads))
    marks = jnp.concatenate(
        [jnp.broadcast_to(largest, (8, rank)), jnp.broadcast_to(rows[8:9, :], (8, rank))], axis=0
    )
    scale = 1.0 / (largest * rows[8:9, :] * term_bound(features))
    other_factor = factor[pl.ds(pl.multiple_of((core ^ 1) * features, features), features), :]
    for k in reversed(range(chips)):
        at = pl.multiple_of(core * half + (chip ^ k) * chunk, chunk)
        part = parts[k * chunk : (k + 1) * chunk, :] + jnp.dot(
            heads[pl.ds(at, chunk), :], other_factor, preferred_element_type=f32
        )
        if k == 0:
            outs[0][...] = part
        else:
            outs[k][0:chunk, :] = part * scale
            outs[k][chunk : chunk + 16, :] = marks
    outs[chips][...] = marks


def term_bound(features):
    return 2 * features / 32768.0


def partial_image(heads, heads_other, factor, chips):
    tokens, _ = heads.shape
    rank = factor.shape[1]
    chunk = tokens // (2 * chips)
    vmem = pl.BlockSpec(memory_space=pltpu.VMEM)
    cost = pl.CostEstimate(flops=200_000_000, bytes_accessed=0, transcendentals=0)
    parts, rows = pl.pallas_call(
        functools.partial(first_kernel, chips),
        out_shape=[
            jax.ShapeDtypeStruct((tokens // 2, rank), f32),
            jax.ShapeDtypeStruct((16, rank), f32),
        ],
        in_specs=[vmem] * 2,
        out_specs=[vmem] * 2,
        compiler_params=SMALL,
        cost_estimate=cost,
        name="partial_first",
    )(heads, factor)
    return pl.pallas_call(
        functools.partial(second_kernel, chips),
        out_shape=[jax.ShapeDtypeStruct((chunk, rank), f32)]
        + [jax.ShapeDtypeStruct((chunk + 16, rank), f32)] * (chips - 1)
        + [jax.ShapeDtypeStruct((16, rank), f32)],
        in_specs=[vmem] * 4,
        out_specs=[vmem] * (chips + 1),
        compiler_params=SMALL,
        cost_estimate=cost,
        name="partial_second",
    )(heads_other, parts, rows, factor)


def pack_kernel(*refs):
    *sources, packed = refs
    at = 0
    for x in sources:
        packed[at : at + x.shape[0], :] = x[...]
        at += x.shape[0]


def pack_rows(*arrays):
    rows = sum(x.shape[0] for x in arrays)
    vmem = pl.BlockSpec(memory_space=pltpu.VMEM)
    return pl.pallas_call(
        pack_kernel,
        out_shape=jax.ShapeDtypeStruct((rows, arrays[0].shape[1]), f32),
        in_specs=[vmem] * len(arrays),
        out_specs=vmem,
        compiler_params=SMALL,
        cost_estimate=pl.CostEstimate(flops=100_000_000, bytes_accessed=0, transcendentals=0),
        name="pack_rows",
    )(*arrays)


def add_kernel(a, b, out):
    out[...] = a[...] + b[...]


def add_tiles(a, b):
    vmem = pl.BlockSpec(memory_space=pltpu.VMEM)
    return pl.pallas_call(
        add_kernel,
        out_shape=jax.ShapeDtypeStruct(a.shape, f32),
        in_specs=[vmem] * 2,
        out_specs=vmem,
        compiler_params=SMALL,
        name="add_tiles",
    )(a, b)


def on_device(
    value_input,
    value_cotangent,
    value_factor,
    value_master,
    value_first,
    value_second,
    mixed_heads,
    output_cotangent,
    output_factor,
    output_master,
    output_first,
    output_second,
):
    fs_count = lax.axis_size("fs")
    tp_count = lax.axis_size("tp")
    tp_place = lax.axis_index("tp")
    chips = tp_count // 2
    core = tp_place & 1
    chip = tp_place >> 1
    rank = value_factor.shape[1]
    columns = value_input.shape[1]
    tokens, features = mixed_heads.shape
    half = tokens // 2
    chunk = half // chips

    def project(image, cotangent):
        return lax.dot_general(
            image,
            cotangent.astype(f32),
            (((0,), (0,)), ((), ())),
            precision=highest,
            preferred_element_type=f32,
        )

    def sum_fs(term):
        own = scaled_term(term).astype(f16)
        terms = [own]
        for k in range(1, fs_count):
            terms.append(send_xor(own, "fs", k))
        sums = []
        for t in terms:
            root = t[rank : rank + 1].astype(f32)
            sums.append(t[:rank].astype(f32) * (root * root * 2.0**-11))
        while len(sums) > 1:
            sums = [sums[2 * i] + sums[2 * i + 1] for i in range(len(sums) // 2)]
        return sums[0]

    def gather_fs(packed, cut):
        if fs_count != 4:
            whole = [packed]
            for k in range(1, fs_count):
                whole.append(send_xor(packed, "fs", k))
            return [(w, 0) for w in whole], [(w, cut) for w in whole]
        near = send_xor(packed, "fs", 1)
        far = send_xor(packed, "fs", 2)
        first = send_xor(near[:cut], "fs", 2)
        last = send_xor(far[cut:], "fs", 1)
        parts = [packed, near, far]
        return [(p, 0) for p in parts] + [(first, 0)], [(p, cut) for p in parts] + [(last, 0)]

    heads_other = send_xor(mixed_heads, "tp", 1)

    value_image = jnp.dot(value_cotangent, value_factor, preferred_element_type=f32)
    value_term = project(value_image, value_input)

    total, *sends, scale_rows = partial_image(
        mixed_heads,
        heads_other,
        lax.dynamic_slice_in_dim(output_factor, chip * (2 * features), 2 * features, 0),
        chips,
    )
    strength = scale_rows[0:1] * scale_rows[8:9]
    arrived = []
    for k in range(1, chips):
        arrived.append(send_xor(sends[k - 1].astype(f16), "tp", 2 * k))
    for a in arrived:
        of_peer = a[chunk : chunk + 1].astype(f32) * a[chunk + 8 : chunk + 9].astype(f32)
        strength = jnp.maximum(strength, of_peer)
        total += a[:chunk].astype(f32) * (term_bound(features) * of_peer)
    bound_total = chips * term_bound(features) * strength
    total = (total * (1.0 / bound_total)).astype(f16)

    products = []
    for k in range(chips):
        mine = send_xor(total, "tp", 2 * k) if k else total
        theirs = send_xor(mine, "tp", 1)
        for at, part in ((core * half, mine), ((1 - core) * half, theirs)):
            rows = lax.dynamic_slice_in_dim(output_cotangent, at + (chip ^ k) * chunk, chunk, 0)
            product = project(part.astype(f32), rows)
            products.append(product)
    output_term = sum(products[1:], products[0]) * bound_total[0, 0]

    value_proj = sum_fs(value_term)
    output_proj = sum_fs(output_term)

    small = (value_first, value_second, output_first, output_second, value_master)
    packed = pack_rows(*small, output_master)
    smalls, larges = gather_fs(packed, sum(x.shape[0] for x in small))

    squares = sum_squares(value_proj, output_proj)
    squares = add_tiles(squares, send_xor(squares, "tp", 1))
    tiles = [squares]
    if chips == 4:
        tiles.append(send_split(squares))
        tiles.append(send_xor(squares, "tp", 4))
        tiles.append(send_xor(tiles[1], "tp", 1))
    else:
        for k in range(1, chips):
            tiles.append(send_xor(squares, "tp", 2 * k))
    return tuple(
        finish(
            tiles,
            1.0 * rank * columns * tp_count,
            value_proj,
            output_proj,
            value_factor,
            output_factor,
            smalls,
            larges,
        )
    )


def solution(mesh):
    in_specs = (
        P("fs", "tp"),
        P("fs", None),
        P(),
        P("fs", "tp"),
        P("fs", "tp"),
        P("fs", "tp"),
        P("fs", "tp"),
        P("fs", "tp"),
        P(),
        P("fs", "tp"),
        P("fs", "tp"),
        P("fs", "tp"),
    )
    out_specs = (
        P("fs", "tp"),
        P("fs", "tp"),
        P(None, "tp"),
        P("fs", "tp"),
        P("fs", "tp"),
        P("fs", "tp"),
        P("fs", "tp"),
        P(None, "tp"),
        P("fs", "tp"),
        P("fs", "tp"),
    )
    return jax.shard_map(
        on_device, mesh=mesh, in_specs=in_specs, out_specs=out_specs, check_vma=False
    )
```

```python
import functools

import jax
import jax.numpy as jnp
from jax import lax
from jax.experimental import pallas as pl
from jax.experimental.pallas import tpu as pltpu
from jax.sharding import PartitionSpec as P


SMALL = pltpu.CompilerParams(vmem_limit_bytes=16 * 2**20)
highest = lax.Precision.HIGH
f32 = jnp.float32
bf16 = jnp.bfloat16
f16 = jnp.float16


def send_xor(x, axis, step):
    count = lax.axis_size(axis)
    return lax.ppermute(x, axis, [(i, i ^ step) for i in range(count)])


def send_split(x):
    return lax.ppermute(x, "tp", [(i, i ^ (6 if i & 1 else 2)) for i in range(8)])


def finish_side(me, scale, projected, blocks, rows, factor, outs, direction, band):
    step_out, new_out, copy_out, first_out, second_out = outs
    for k, (first_old, second_old, _) in enumerate(blocks):
        at = pl.multiple_of((me ^ k) * band, band)
        scaled = scale * projected[pl.ds(at, band), :]
        first = 0.9 * first_old[...] + 0.1 * scaled
        second = 0.95 * second_old[...] + 0.05 * scaled * scaled
        if k == 0:
            first_out[...] = first
            second_out[...] = second
        direction[pl.ds(at, band), :] = first / (jnp.sqrt(second) + 1e-08)
    high = direction[...].astype(bf16)
    low = (direction[...] - high.astype(f32)).astype(bf16)
    for k, (_, _, master) in enumerate(blocks):
        at = pl.multiple_of((me ^ k) * rows, rows)
        own = factor[pl.ds(at, rows), :]
        step = jnp.dot(own, high, preferred_element_type=f32) + jnp.dot(
            own, low, preferred_element_type=f32
        )
        new = master[...] - 0.002 * step
        copy_out[pl.ds(at, rows), :] = new.astype(bf16)
        if k == 0:
            step_out[...] = step
            new_out[...] = new


def finish_kernel(chips, places, entries, value_rows, output_rows, *refs):
    tiles, refs = refs[:chips], refs[chips:]
    value_proj, output_proj, value_factor, output_factor = refs[:4]
    outs, direction = refs[-11:-1], refs[-1]
    packs = refs[4:-11]
    me = lax.axis_index("fs")
    sums = [t[0:1, :] for t in tiles]
    while len(sums) > 1:
        sums = [sums[2 * i] + sums[2 * i + 1] for i in range(len(sums) // 2)]
    scales = lax.rsqrt(sums[0] / entries + 1e-06)
    band = direction.shape[0] // len(places)
    value_blocks, output_blocks = [], []
    for (small, at), (large, at_large) in places:
        cuts = [packs[small].at[at + i * band : at + (i + 1) * band, :] for i in range(4)]
        value_master = packs[small].at[at + 4 * band : at + 4 * band + value_rows, :]
        output_master = packs[large].at[at_large : at_large + output_rows, :]
        value_blocks.append((cuts[0], cuts[1], value_master))
        output_blocks.append((cuts[2], cuts[3], output_master))
    for scale, projected, blocks, rows, factor, side_outs in (
        (scales[:, 0:1], value_proj, value_blocks, value_rows, value_factor, outs[:5]),
        (scales[:, 64:65], output_proj, output_blocks, output_rows, output_factor, outs[5:]),
    ):
        finish_side(me, scale, projected, blocks, rows, factor, side_outs, direction, band)


def finish(tiles, entries, value_proj, output_proj, value_factor, output_factor, smalls, larges):
    count = len(smalls)
    rank, columns = value_proj.shape
    band = rank // count
    value_rows, output_rows = value_factor.shape[0] // count, output_factor.shape[0] // count
    vmem = pl.BlockSpec(memory_space=pltpu.VMEM)
    arrays = []

    def place(part):
        array, at = part
        for i, known in enumerate(arrays):
            if known is array:
                return i, at
        arrays.append(array)
        return len(arrays) - 1, at

    places = tuple((place(small), place(large)) for small, large in zip(smalls, larges))

    def side(rows):
        return [
            jax.ShapeDtypeStruct((rows, columns), f32),
            jax.ShapeDtypeStruct((rows, columns), f32),
            jax.ShapeDtypeStruct((rows * count, columns), bf16),
            jax.ShapeDtypeStruct((band, columns), f32),
            jax.ShapeDtypeStruct((band, columns), f32),
        ]

    return pl.pallas_call(
        functools.partial(finish_kernel, len(tiles), places, entries, value_rows, output_rows),
        out_shape=side(value_rows) + side(output_rows),
        in_specs=[vmem] * (len(tiles) + 4 + len(arrays)),
        out_specs=[vmem] * 10,
        scratch_shapes=[pltpu.VMEM((rank, columns), f32)],
        compiler_params=SMALL,
        name="finish",
    )(*tiles, value_proj, output_proj, value_factor, output_factor, *arrays)


def term_kernel(x, out):
    rank, columns = x.shape
    root = jnp.maximum(jnp.sqrt(largest_of(x)) * 0.25, 2.0**-14)
    wide = root * (2.0**23 + 1.0)
    root = 2.0 * (wide - (wide - root))
    out[0:rank, :] = x[...] * (2048.0 / (root * root))
    out[rank : rank + 16, :] = jnp.broadcast_to(root, (16, columns))


def scaled_term(x):
    vmem = pl.BlockSpec(memory_space=pltpu.VMEM)
    rank, columns = x.shape
    return pl.pallas_call(
        term_kernel,
        out_shape=jax.ShapeDtypeStruct((rank + 16, columns), f32),
        in_specs=[vmem],
        out_specs=vmem,
        compiler_params=SMALL,
        cost_estimate=pl.CostEstimate(flops=100_000_000, bytes_accessed=0, transcendentals=0),
        name="scaled_term",
    )(x)


def square_kernel(value, output, squares):
    def square(x):
        return jnp.sum(jnp.sum(x * x, axis=0, keepdims=True), axis=1, keepdims=True)

    lane = lax.broadcasted_iota(jnp.int32, squares.shape, 1)
    squares[...] = jnp.where(lane < 64, square(value[...]), square(output[...]))


def sum_squares(value, output):
    vmem = pl.BlockSpec(memory_space=pltpu.VMEM)
    return pl.pallas_call(
        square_kernel,
        out_shape=jax.ShapeDtypeStruct((8, 128), f32),
        in_specs=[vmem] * 2,
        out_specs=vmem,
        compiler_params=SMALL,
        cost_estimate=pl.CostEstimate(flops=100_000_000, bytes_accessed=0, transcendentals=0),
        name="sum_squares",
    )(value, output)


def largest_of(x):
    return jnp.max(jnp.max(jnp.abs(x[...]).astype(f32), axis=0, keepdims=True), axis=1, keepdims=True)


def chunks_of(core, chip, chips, half, chunk):
    offsets = [core * half + (chip ^ k) * chunk for k in range(chips)]
    if chips == 4:
        split = (chip ^ (1 + 2 * core)) * chunk
        offsets = [offsets[0], core * half + split, (1 - core) * half + split, offsets[2]]
    return [pl.multiple_of(at, chunk) for at in offsets]


def first_kernel(chips, heads, factor, parts, rows_out):
    tokens, features = heads.shape
    half, rank = tokens // 2, factor.shape[1]
    chunk = half // chips
    place = lax.axis_index("tp")
    core, chip = place & 1, place >> 1
    own_factor = factor[pl.ds(pl.multiple_of(core * features, features), features), :]
    for k, at in enumerate(chunks_of(core, chip, chips, half, chunk)):
        parts[k * chunk : (k + 1) * chunk, :] = jnp.dot(
            heads[pl.ds(at, chunk), :], own_factor, preferred_element_type=f32
        )
    rows_out[0:8, :] = jnp.broadcast_to(jnp.maximum(largest_of(heads), 2.0**-13), (8, rank))
    rows_out[8:16, :] = jnp.broadcast_to(jnp.maximum(largest_of(factor), 2.0**-13), (8, rank))


def second_kernel(chips, heads, parts, rows, factor, *outs):
    tokens, features = heads.shape
    half, rank = tokens // 2, factor.shape[1]
    chunk = half // chips
    place = lax.axis_index("tp")
    core, chip = place & 1, place >> 1
    largest = jnp.maximum(rows[0:1, :], largest_of(heads))
    marks = jnp.concatenate(
        [jnp.broadcast_to(largest, (8, rank)), jnp.broadcast_to(rows[8:9, :], (8, rank))], axis=0
    )
    scale = 1.0 / (largest * rows[8:9, :] * term_bound(features))
    other_factor = factor[pl.ds(pl.multiple_of((core ^ 1) * features, features), features), :]
    own, *sends, marks_out = outs
    places = [(0, 0), (0, chunk), (1, 0)] if chips == 4 else [(k, 0) for k in range(chips - 1)]
    for k, at in enumerate(chunks_of(core, chip, chips, half, chunk)):
        part = parts[k * chunk : (k + 1) * chunk, :] + jnp.dot(
            heads[pl.ds(at, chunk), :], other_factor, preferred_element_type=f32
        )
        if k == 0:
            own[...] = part
        else:
            which, row = places[k - 1]
            sends[which][row : row + chunk, :] = part * scale
    for send in sends:
        send[send.shape[0] - 16 : send.shape[0], :] = marks
    marks_out[...] = marks


def term_bound(features):
    return 2 * features / 32768.0


def partial_image(heads, heads_other, factor, chips):
    tokens, _ = heads.shape
    rank = factor.shape[1]
    chunk = tokens // (2 * chips)
    lengths = [2 * chunk + 16, chunk + 16] if chips == 4 else [chunk + 16] * (chips - 1)
    vmem = pl.BlockSpec(memory_space=pltpu.VMEM)
    cost = pl.CostEstimate(flops=200_000_000, bytes_accessed=0, transcendentals=0)
    parts, rows = pl.pallas_call(
        functools.partial(first_kernel, chips),
        out_shape=[
            jax.ShapeDtypeStruct((tokens // 2, rank), f32),
            jax.ShapeDtypeStruct((16, rank), f32),
        ],
        in_specs=[vmem] * 2,
        out_specs=[vmem] * 2,
        compiler_params=SMALL,
        cost_estimate=cost,
        name="partial_first",
    )(heads, factor)
    return pl.pallas_call(
        functools.partial(second_kernel, chips),
        out_shape=[jax.ShapeDtypeStruct((n, rank), f32) for n in (chunk, *lengths, 16)],
        in_specs=[vmem] * 4,
        out_specs=[vmem] * (2 + len(lengths)),
        compiler_params=SMALL,
        cost_estimate=cost,
        name="partial_second",
    )(heads_other, parts, rows, factor)


def pack_kernel(*refs):
    *sources, packed = refs
    at = 0
    for x in sources:
        packed[at : at + x.shape[0], :] = x[...]
        at += x.shape[0]


def pack_rows(*arrays):
    rows = sum(x.shape[0] for x in arrays)
    vmem = pl.BlockSpec(memory_space=pltpu.VMEM)
    return pl.pallas_call(
        pack_kernel,
        out_shape=jax.ShapeDtypeStruct((rows, arrays[0].shape[1]), f32),
        in_specs=[vmem] * len(arrays),
        out_specs=vmem,
        compiler_params=SMALL,
        cost_estimate=pl.CostEstimate(flops=100_000_000, bytes_accessed=0, transcendentals=0),
        name="pack_rows",
    )(*arrays)


def add_kernel(a, b, out):
    out[...] = a[...] + b[...]


def add_tiles(a, b):
    vmem = pl.BlockSpec(memory_space=pltpu.VMEM)
    return pl.pallas_call(
        add_kernel,
        out_shape=jax.ShapeDtypeStruct(a.shape, f32),
        in_specs=[vmem] * 2,
        out_specs=vmem,
        compiler_params=SMALL,
        name="add_tiles",
    )(a, b)


def on_device(
    value_input,
    value_cotangent,
    value_factor,
    value_master,
    value_first,
    value_second,
    mixed_heads,
    output_cotangent,
    output_factor,
    output_master,
    output_first,
    output_second,
):
    fs_count = lax.axis_size("fs")
    tp_count = lax.axis_size("tp")
    tp_place = lax.axis_index("tp")
    chips = tp_count // 2
    core = tp_place & 1
    chip = tp_place >> 1
    rank = value_factor.shape[1]
    columns = value_input.shape[1]
    tokens, features = mixed_heads.shape
    half = tokens // 2
    chunk = half // chips

    def project(image, cotangent):
        return lax.dot_general(
            image,
            cotangent.astype(f32),
            (((0,), (0,)), ((), ())),
            precision=highest,
            preferred_element_type=f32,
        )

    def sum_fs(term):
        own = scaled_term(term).astype(f16)
        terms = [own]
        for k in range(1, fs_count):
            terms.append(send_xor(own, "fs", k))
        sums = []
        for t in terms:
            root = t[rank : rank + 1].astype(f32)
            sums.append(t[:rank].astype(f32) * (root * root * 2.0**-11))
        while len(sums) > 1:
            sums = [sums[2 * i] + sums[2 * i + 1] for i in range(len(sums) // 2)]
        return sums[0]

    def gather_fs(packed, cut):
        if fs_count != 4:
            whole = [packed]
            for k in range(1, fs_count):
                whole.append(send_xor(packed, "fs", k))
            return [(w, 0) for w in whole], [(w, cut) for w in whole]
        near = send_xor(packed, "fs", 1)
        far = send_xor(packed, "fs", 2)
        first = send_xor(near[:cut], "fs", 2)
        last = send_xor(far[cut:], "fs", 1)
        parts = [packed, near, far]
        return [(p, 0) for p in parts] + [(first, 0)], [(p, cut) for p in parts] + [(last, 0)]

    heads_other = send_xor(mixed_heads, "tp", 1)

    value_image = jnp.dot(value_cotangent, value_factor, preferred_element_type=f32)
    value_term = project(value_image, value_input)

    total, *sends, scale_rows = partial_image(
        mixed_heads,
        heads_other,
        lax.dynamic_slice_in_dim(output_factor, chip * (2 * features), 2 * features, 0),
        chips,
    )
    strength = scale_rows[0:1] * scale_rows[8:9]
    arrived = []
    sends = [send.astype(f16) for send in sends]
    if chips == 4:
        halves = send_split(sends[0])
        arrived.append(send_xor(sends[1], "tp", 4))
        arrived.append(send_xor(halves[chunk:], "tp", 1))
        arrived.append(jnp.concatenate([halves[:chunk], halves[2 * chunk :]], axis=0))
    else:
        for k in range(1, chips):
            arrived.append(send_xor(sends[k - 1], "tp", 2 * k))
    for a in arrived:
        of_peer = a[chunk : chunk + 1].astype(f32) * a[chunk + 8 : chunk + 9].astype(f32)
        strength = jnp.maximum(strength, of_peer)
        total += a[:chunk].astype(f32) * (term_bound(features) * of_peer)
    bound_total = chips * term_bound(features) * strength
    total = (total * (1.0 / bound_total)).astype(f16)

    def product(part, at):
        rows = lax.dynamic_slice_in_dim(output_cotangent, at, chunk, 0)
        return project(part.astype(f32), rows)

    here, there = core * half, (1 - core) * half
    theirs = send_xor(total, "tp", 1)
    products = [product(total, here + chip * chunk)]
    products.append(product(theirs, there + chip * chunk))
    for k in range(1, chips):
        mine = send_xor(total, "tp", 2 * k)
        theirs = send_xor(mine, "tp", 1)
        products.append(product(mine, here + (chip ^ k) * chunk))
        products.append(product(theirs, there + (chip ^ k) * chunk))
    output_term = sum(products[1:], products[0]) * bound_total[0, 0]

    value_proj = sum_fs(value_term)
    output_proj = sum_fs(output_term)

    small = (value_first, value_second, output_first, output_second, value_master)
    packed = pack_rows(*small, output_master)
    smalls, larges = gather_fs(packed, sum(x.shape[0] for x in small))

    squares = sum_squares(value_proj, output_proj)
    squares = add_tiles(squares, send_xor(squares, "tp", 1))
    tiles = [squares]
    if chips == 4:
        tiles.append(send_split(squares))
        tiles.append(send_xor(squares, "tp", 4))
        tiles.append(send_xor(tiles[1], "tp", 1))
    else:
        for k in range(1, chips):
            tiles.append(send_xor(squares, "tp", 2 * k))
    return tuple(
        finish(
            tiles,
            1.0 * rank * columns * tp_count,
            value_proj,
            output_proj,
            value_factor,
            output_factor,
            smalls,
            larges,
        )
    )


def solution(mesh):
    in_specs = (
        P("fs", "tp"),
        P("fs", None),
        P(),
        P("fs", "tp"),
        P("fs", "tp"),
        P("fs", "tp"),
        P("fs", "tp"),
        P("fs", "tp"),
        P(),
        P("fs", "tp"),
        P("fs", "tp"),
        P("fs", "tp"),
    )
    out_specs = (
        P("fs", "tp"),
        P("fs", "tp"),
        P(None, "tp"),
        P("fs", "tp"),
        P("fs", "tp"),
        P("fs", "tp"),
        P("fs", "tp"),
        P(None, "tp"),
        P("fs", "tp"),
        P("fs", "tp"),
    )
    return jax.shard_map(
        on_device, mesh=mesh, in_specs=in_specs, out_specs=out_specs, check_vma=False
    )
```
